32 devices in a mesh: kv: 8 (over z, y), tp: 4 (over x, core).
Axes of the slice: x: 2, y: 2, z: 4, core: 2. Of those that a mesh axis runs over, the one named last changes fastest.
Arguments:
- tokens: bfloat16 [256, 4, 2048], P(None, None, ('kv', 'tp')), may hold values from -520 to 520
- input_norm_gain: bfloat16 [2048], replicated, may hold values from 0.099609375 to 1.8984375
- query_weight: bfloat16 [2048, 2048], P(None, 'kv'), may hold values from -0.125 to 0.125
- key_weight: bfloat16 [2048, 2048], P(None, 'kv'), may hold values from -0.125 to 0.125
- value_weight: bfloat16 [2048, 16, 128], P(None, 'kv', 'tp'), may hold values from -1.14904852 to 1.14904852
- output_gate_weight: bfloat16 [2048, 16, 128], P(None, 'kv', 'tp'), may hold values from -0.125 to 0.125
- strength_weight: bfloat16 [2048, 16], P(None, 'kv'), may hold values from -0.125 to 0.125
- decay_weight: bfloat16 [2048, 16], P(None, 'kv'), may hold values from -0.125 to 0.125
- head_decay_rate: float32 [16], P('kv'), may hold values from 0.005 to 1.5
- proposal_log_decay: float32 [256, 4, 16], P(None, None, 'kv'), may hold values from -0.69 to 0
- head_norm_gain: bfloat16 [128], P('tp'), may hold values from 0.099609375 to 1.8984375
- output_weight: bfloat16 [16, 128, 2048], P('kv', 'tp'), may hold values from -1.14904852 to 1.14904852
- output_norm_gain: bfloat16 [2048], P(('kv', 'tp')), may hold values from 0.099609375 to 1.8984375
- state: float32 [256, 16, 128, 128], P(None, 'kv', 'tp'), may hold values from -4.5961941 to 4.5961941
- previous_keys: bfloat16 [256, 4, 2048], P(None, None, 'kv'), may hold values from -6 to 6
- previous_values: bfloat16 [256, 4, 16, 128], P(None, None, 'kv', 'tp'), may hold values from -52 to 52
- previous_log_decay: float32 [256, 4, 16], P(None, None, 'kv'), may hold values from -0.7 to -0.02
- previous_strengths: float32 [256, 4, 16], P(None, None, 'kv'), may hold values from 0.1 to 0.9
- accepted: int32 [256], replicated, may hold values from 0 to 4
- parent: int32 [256, 4], replicated, may hold values from -1 to 2, as said below
Outputs:
- layer_out: bfloat16 [256, 4, 2048], P(None, None, ('kv', 'tp'))
- accepted_state: float32 [256, 16, 128, 128], P(None, 'kv', 'tp')
The draws below stay inside these ranges and needn't reach their ends.
Inputs may be any that keep to these rules, and one draw needn't show every extreme that they name: parent[b, i] is -1 or a proposal index below i; -1 means that proposal i follows the accepted old proposals directly.
All inputs are finite; a program needn't handle non-finite values.
Results may differ from the reference program's by a relative error of at most 0.019.
Values may be sent and summed in bfloat16 or wider, within the bound.
A program may use at most 128 MiB of HBM per device.

```python
import jax
import jax.numpy as jnp
from jax import lax

D = 2048
H = 16
HD = 128
PROP = 4
SEQS = 256


def column_scales(key, count):
    position = jnp.arange(count, dtype=jnp.float32) / max(count - 1, 1)
    spread = jax.random.uniform(key, (count,), jnp.float32)
    return jnp.exp(jnp.log(3.0) * position + jnp.log(3.4) * spread)


def rough_base(key, shape):
    base = jax.random.normal(key, shape, jnp.float32)
    return jnp.clip(base, -5.0, 5.0)


def draw_tokens(key, part):
    subkeys = jax.random.split(jax.random.fold_in(key, 11), 3)
    base = rough_base(subkeys[0], (SEQS, PROP, D))
    rowscale = jnp.exp(jnp.log(10.0) * jax.random.uniform(subkeys[2], (SEQS, PROP, 1), jnp.float32))
    return (base * column_scales(subkeys[1], D)[None, None, :] * rowscale).astype(jnp.bfloat16)


def draw_output_weight(key, part):
    subkeys = jax.random.split(jax.random.fold_in(key, 23), 2)
    base = jax.random.normal(subkeys[0], (H, HD, D), jnp.float32)
    base = jnp.clip(base, -5.0, 5.0)
    scaled = base * (H * HD) ** (-0.5) * column_scales(subkeys[1], D)[None, None, :]
    return scaled.astype(jnp.bfloat16)


def draw_value_weight(key, part):
    subkeys = jax.random.split(jax.random.fold_in(key, 61), 2)
    base = rough_base(subkeys[0], (D, H, HD))
    return (base * D ** (-0.5) * column_scales(subkeys[1], HD)[None, None, :]).astype(jnp.bfloat16)


def draw_state(key, part):
    subkeys = jax.random.split(jax.random.fold_in(key, 67), 2)
    base = rough_base(subkeys[0], (SEQS, H, HD, HD))
    return base * HD ** (-0.5) * column_scales(subkeys[1], HD)[None, None, :, None]


def draw_previous_values(key, part):
    subkeys = jax.random.split(jax.random.fold_in(key, 71), 2)
    base = rough_base(subkeys[0], (SEQS, PROP, H, HD))
    return (base * column_scales(subkeys[1], HD)[None, None, None, :]).astype(jnp.bfloat16)


def draw_head_decay_rate(key, part):
    uniform_part = jax.random.uniform(jax.random.fold_in(key, 31), (H,), jnp.float32)
    lowest = 0.02
    highest = 1.5
    return jnp.exp(jnp.log(lowest) + uniform_part * (jnp.log(highest) - jnp.log(lowest)))


def draw_proposal_log_decay(key, part):
    subkeys = jax.random.split(jax.random.fold_in(key, 41), 2)
    chosen = (jax.random.randint(subkeys[0], (SEQS, PROP, H), 0, 4) == 0).astype(jnp.float32)
    depth = jax.random.uniform(subkeys[1], (SEQS, PROP, H), jnp.float32, 0.22, 0.69)
    return -depth * chosen


def draw_parent(key, part):
    raw_bits = jax.random.randint(jax.random.fold_in(key, 53), (SEQS, PROP), 0, 1 << 20)
    column = jnp.arange(PROP, dtype=jnp.int32)
    return (raw_bits % (column[None, :] + 1) - 1).astype(jnp.int32)


def set_ends(drawn, rng, low, top_value):
    extent = drawn.shape
    spot = [jax.random.randint(jax.random.fold_in(rng, axis), (), 0, extent[axis]) for axis in range(len(extent))]
    drawn = drawn.at[tuple(spot)].set(low)
    longest = extent.index(max(extent))
    spot[longest] = (spot[longest] + 1) % extent[longest]
    return drawn.at[tuple(spot)].set(top_value)


def levels(own_key, shape, shards, smallest, high):
    gain, own = 1.0, jax.random.fold_in(own_key, 6)
    for dim, parts in shards:
        draws = jnp.exp(jax.random.uniform(jax.random.fold_in(own, dim), (parts,), jnp.float32, smallest / len(shards), high / len(shards)))
        gain = gain * jnp.repeat(draws, shape[dim] // parts).reshape([-1 if axis == dim else 1 for axis in range(len(shape))])
    return gain


def normal_values(own_key, extent, scale, most, cuts=(), kind=jnp.bfloat16):
    values = scale * jax.random.normal(own_key, extent, jnp.float32)
    if cuts:
        values = values * levels(own_key, extent, cuts, -0.22, 0.18)
    return jnp.clip(values, -most, most).astype(kind)


def setup_inputs(seed: int = 0) -> dict:
    key_list = jax.random.split(jax.random.key(seed), 21)
    tokens = draw_tokens(jax.random.fold_in(key_list[20], 71), 0)
    input_norm_gain = jnp.clip(1.0 + 0.18 * jax.random.normal(key_list[1], (D,), jnp.float32), 0.099609375, 1.8984375).astype(jnp.bfloat16)
    query_weight = normal_values(key_list[2], (D, H * HD), D ** -0.5, 0.125, ((1, 8),))
    key_weight = normal_values(key_list[3], (D, H * HD), D ** -0.5, 0.125, ((1, 8),))
    value_weight = draw_value_weight(jax.random.fold_in(key_list[20], 71), 0)
    output_gate_weight = normal_values(key_list[5], (D, H, HD), D ** -0.5, 0.125, ((1, 8), (2, 4)))
    strength_weight = normal_values(key_list[6], (D, H), D ** -0.5, 0.125, ((1, 8),))
    decay_weight = normal_values(key_list[7], (D, H), D ** -0.5, 0.125, ((1, 8),))
    head_decay_rate = draw_head_decay_rate(jax.random.fold_in(key_list[20], 71), 0)
    proposal_log_decay = draw_proposal_log_decay(jax.random.fold_in(key_list[20], 71), 0)
    head_norm_gain = jnp.clip(1.0 + 0.18 * jax.random.normal(key_list[10], (HD,), jnp.float32), 0.099609375, 1.8984375).astype(jnp.bfloat16)
    output_weight = draw_output_weight(jax.random.fold_in(key_list[20], 71), 0)
    output_norm_gain = jnp.clip(1.0 + 0.18 * jax.random.normal(key_list[12], (D,), jnp.float32), 0.099609375, 1.8984375).astype(jnp.bfloat16)
    state = draw_state(jax.random.fold_in(key_list[20], 71), 0)
    previous_keys = normal_values(key_list[14], (SEQS, PROP, H * HD), 1.0, 6.0, ((2, 8),))
    previous_values = draw_previous_values(jax.random.fold_in(key_list[20], 71), 0)
    previous_log_decay = jnp.clip(-0.7 + 0.68 * jax.random.uniform(key_list[16], (SEQS, PROP, H), jnp.float32) ** levels(key_list[16], (SEQS, PROP, H), ((2, 8),), -0.2, 0.2), -0.7, -0.02)
    previous_strengths = jnp.clip(0.1 + 0.79999997 * jax.random.uniform(key_list[17], (SEQS, PROP, H), jnp.float32) ** levels(key_list[17], (SEQS, PROP, H), ((2, 8),), -0.2, 0.2), 0.1, 0.9)
    accepted = set_ends(jax.random.randint(key_list[18], (SEQS,), 0, PROP + 1), jax.random.fold_in(key_list[18], 1), 0, PROP).astype(jnp.int32)
    parent = draw_parent(jax.random.fold_in(key_list[20], 71), 0)
    return {"tokens": tokens, "input_norm_gain": input_norm_gain, "query_weight": query_weight, "key_weight": key_weight, "value_weight": value_weight, "output_gate_weight": output_gate_weight, "strength_weight": strength_weight, "decay_weight": decay_weight, "head_decay_rate": head_decay_rate, "proposal_log_decay": proposal_log_decay, "head_norm_gain": head_norm_gain, "output_weight": output_weight, "output_norm_gain": output_norm_gain, "state": state, "previous_keys": previous_keys, "previous_values": previous_values, "previous_log_decay": previous_log_decay, "previous_strengths": previous_strengths, "accepted": accepted, "parent": parent}


epsilon = 1e-06

def unit_rows(matrix):
    return matrix * lax.rsqrt(lax.optimization_barrier(jnp.sum(matrix * matrix, axis=-1, keepdims=True)) + epsilon)

def exact_product(form, left, right):
    return jnp.einsum(form, left, right, precision=lax.Precision.HIGHEST)

def visibility(parent):
    sequence_count, proposal_count = parent.shape
    position = jnp.arange(proposal_count, dtype=jnp.int32)
    parent_hot = (parent[:, :, None] == position[None, None, :]).astype(jnp.float32)
    ancestry = []
    for row_index in range(proposal_count):
        ancestor_row = parent_hot[:, row_index, :]
        if row_index > 0:
            earlier = jnp.stack(ancestry, axis=1)
            ancestor_row = ancestor_row + exact_product('bj,bjk->bk', parent_hot[:, row_index, :row_index], earlier)
        ancestry.append(ancestor_row)
    ancestor = jnp.stack(ancestry, axis=1)
    chain = (position[:, None] > position[None, :]).astype(jnp.float32)
    upper = jnp.concatenate([jnp.broadcast_to(chain, (sequence_count, proposal_count, proposal_count)), jnp.zeros((sequence_count, proposal_count, proposal_count), jnp.float32)], axis=2)
    lower = jnp.concatenate([jnp.ones((sequence_count, proposal_count, proposal_count), jnp.float32), ancestor], axis=2)
    return jnp.concatenate([upper, lower], axis=1)

def split_heads(matrix, sequence_count, proposal_count, number_of_heads):
    return matrix.astype(jnp.float32).reshape(sequence_count, proposal_count, number_of_heads, -1).transpose(0, 2, 1, 3)

def delta_recursion(query_projected, key_projected, value_projected, output_gate_logits, write_strength_logits, decay_logits, decay_speed, proposal_group, head_norm_gain, state, previous_keys, previous_values, previous_log_decay, previous_strengths, accepted, parent, channel_count_total):
    sequence_count, number_of_heads, value_dim, head_dim = state.shape
    proposal_count = parent.shape[1]
    queries = unit_rows(split_heads(query_projected, sequence_count, proposal_count, number_of_heads)) * head_dim ** (-0.5)
    new_keys = unit_rows(split_heads(key_projected, sequence_count, proposal_count, number_of_heads))
    old_keys = unit_rows(split_heads(previous_keys, sequence_count, proposal_count, number_of_heads))
    new_values = split_heads(value_projected, sequence_count, proposal_count, number_of_heads)
    old_values = split_heads(previous_values, sequence_count, proposal_count, number_of_heads)
    zgate = split_heads(output_gate_logits, sequence_count, proposal_count, number_of_heads)
    beta_new = jax.nn.sigmoid(write_strength_logits.reshape(sequence_count, proposal_count, number_of_heads)).transpose(0, 2, 1)
    fresh_decay = (-decay_speed[None, None, :] * jax.nn.softplus(decay_logits.reshape(sequence_count, proposal_count, number_of_heads)) + proposal_group).transpose(0, 2, 1)
    position = jnp.arange(proposal_count, dtype=jnp.int32)
    live = (position[None, :] < accepted[:, None]).astype(jnp.float32)[:, None, :]
    beta_old = previous_strengths.transpose(0, 2, 1) * live
    decay_old = previous_log_decay.transpose(0, 2, 1) * live
    keys_all = jnp.concatenate([old_keys, new_keys], axis=2)
    values_all = jnp.concatenate([old_values, new_values], axis=2)
    beta_all = jnp.concatenate([beta_old, beta_new], axis=2)
    decay_all = jnp.concatenate([decay_old, fresh_decay], axis=2)
    visible = visibility(parent)
    gamma_sum = decay_all + exact_product('bij,bhj->bhi', visible, decay_all)
    gamma_diff = gamma_sum[:, :, :, None] - gamma_sum[:, :, None, :]
    decay_pair = jnp.exp(jnp.minimum(gamma_diff, 0.0)) * visible[:, None]
    coupling = beta_all[..., None] * exact_product('bhid,bhjd->bhij', keys_all, keys_all) * decay_pair
    right_side = jnp.concatenate([beta_all[..., None] * values_all, (beta_all * jnp.exp(gamma_sum))[..., None] * keys_all], axis=-1)
    solved = []
    for row_index in range(2 * proposal_count):
        current = right_side[:, :, row_index]
        if row_index > 0:
            current = current - exact_product('bhj,bhjd->bhd', coupling[:, :, row_index, :row_index], jnp.stack(solved, axis=2))
        solved.append(current)
    solution = jnp.stack(solved, axis=2)
    update = solution[..., :value_dim] - exact_product('bhcd,bhed->bhce', solution[..., value_dim:], state)
    identity = jnp.eye(2 * proposal_count, dtype=jnp.float32)
    seen = visible[:, proposal_count:] + identity[proposal_count:][None]
    reach = jnp.exp(jnp.minimum(gamma_diff[:, :, proposal_count:], 0.0)) * seen[:, None]
    query_key = exact_product('bhid,bhjd->bhij', queries, keys_all) * reach
    readout = exact_product('bhid,bhed->bhie', queries * jnp.exp(gamma_sum[:, :, proposal_count:])[..., None], state)
    readout = readout + exact_product('bhij,bhje->bhie', query_key, update)
    squares = channel_count_total(lax.optimization_barrier(jnp.sum(readout * readout, axis=-1)))
    readout = readout * lax.rsqrt(squares / head_dim + epsilon)[..., None]
    readout = readout * head_norm_gain.astype(jnp.float32) * jax.nn.silu(zgate)
    blended_rows = readout.transpose(0, 2, 1, 3).reshape(sequence_count * proposal_count, number_of_heads * value_dim)
    blended_rows = blended_rows.astype(jnp.bfloat16)
    last_gamma = gamma_sum[:, :, proposal_count - 1:proposal_count]
    key_weighted = old_keys * jnp.exp(last_gamma - gamma_sum[:, :, :proposal_count])[..., None]
    accepted_state = jnp.exp(last_gamma)[..., None] * state + exact_product('bhcd,bhce->bhed', key_weighted, update[:, :, :proposal_count])
    return (blended_rows, accepted_state)

def kept_channel_total(squares):
    return squares

def reference(tokens, input_norm_gain, query_weight, key_weight, value_weight, output_gate_weight, strength_weight, decay_weight, head_decay_rate, proposal_log_decay, head_norm_gain, output_weight, output_norm_gain, state, previous_keys, previous_values, previous_log_decay, previous_strengths, accepted, parent):
    sequence_count, proposal_count, width = tokens.shape
    features = tokens.astype(jnp.float32)
    normed = features * lax.rsqrt(lax.optimization_barrier(jnp.mean(features * features, axis=-1, keepdims=True)) + epsilon)
    normed = (normed * input_norm_gain.astype(jnp.float32)).astype(jnp.bfloat16)
    flat_rows = normed.reshape(sequence_count * proposal_count, width)
    query_projected = jnp.dot(flat_rows, query_weight, preferred_element_type=jnp.float32).astype(jnp.bfloat16)
    key_projected = jnp.dot(flat_rows, key_weight, preferred_element_type=jnp.float32).astype(jnp.bfloat16)
    value_projected = jnp.dot(flat_rows, value_weight.reshape(width, -1), preferred_element_type=jnp.float32).astype(jnp.bfloat16)
    output_gate_logits = jnp.dot(flat_rows, output_gate_weight.reshape(width, -1), preferred_element_type=jnp.float32).astype(jnp.bfloat16)
    write_strength_logits = jnp.dot(flat_rows, strength_weight, preferred_element_type=jnp.float32)
    decay_logits = jnp.dot(flat_rows, decay_weight, preferred_element_type=jnp.float32)
    blended_rows, accepted_state = delta_recursion(query_projected, key_projected, value_projected, output_gate_logits, write_strength_logits, decay_logits, head_decay_rate, proposal_log_decay, head_norm_gain, state, previous_keys, previous_values, previous_log_decay, previous_strengths, accepted, parent, kept_channel_total)
    combined = jnp.dot(blended_rows, output_weight.reshape(-1, width), preferred_element_type=jnp.float32)
    combined = combined * lax.rsqrt(lax.optimization_barrier(jnp.mean(combined * combined, axis=-1, keepdims=True)) + epsilon)
    layer_out = (combined * output_norm_gain.astype(jnp.float32)).astype(jnp.bfloat16).reshape(sequence_count, proposal_count, width)
    return (layer_out, accepted_state)
```

```python
import functools

import jax
import jax.numpy as jnp
from jax import lax
from jax.experimental import pallas as pl
from jax.experimental.pallas import tpu as pltpu
from jax.sharding import PartitionSpec as P

epsilon = 1e-06
GROUP = 16
AXES = ("kv", "tp")


def total(terms):
    terms = list(terms)
    while len(terms) > 1:
        terms = [sum(terms[i : i + 2][1:], terms[i]) for i in range(0, len(terms), 2)]
    return terms[0]


def delta_kernel(
    prop, q_ref, k_ref, ok_ref, v_ref, ov_ref, sc_ref, s_ref, o_ref, sq_ref, out_ref, kt_ref, eg_ref
):
    lanes = s_ref.shape[0]
    vdim = s_ref.shape[2]
    hd = s_ref.shape[3]
    groups = lanes // GROUP
    f32, bf16 = jnp.float32, jnp.bfloat16

    for index, ref in enumerate((ok_ref, k_ref, q_ref)):
        for p in range(prop):
            tile = ref[p * lanes : (p + 1) * lanes, :].astype(f32)
            kt_ref[index * prop + p] = tile.T
    positions = 2 * prop
    square = [jnp.sum(kt_ref[i] * kt_ref[i], axis=0, keepdims=True) for i in range(3 * prop)]
    inv = [lax.rsqrt(x + epsilon) for x in square]
    inv = inv[:positions] + [x * hd ** (-0.5) for x in inv[positions:]]

    def scalar(row, p):
        return sc_ref[0, row : row + 1, p * lanes : (p + 1) * lanes]

    beta = [scalar(0, p) for p in range(prop)] + [scalar(2, p) for p in range(prop)]
    g = [scalar(1, p) for p in range(prop)] + [scalar(3, p) for p in range(prop)]
    parents = [scalar(4, p) for p in range(prop)]
    ancestor = []
    for i in range(prop):
        direct = [jnp.where(parents[i] == float(j), 1.0, 0.0) for j in range(i)]
        row = []
        for j in range(i):
            row.append(total([direct[j]] + [direct[m] * ancestor[m][j] for m in range(j + 1, i)]))
        ancestor.append(row)

    def vis(i, j):
        if i < prop or j < prop:
            return None
        return ancestor[i - prop][j - prop]

    gam = []
    for i in range(positions):
        acc = g[i]
        for j in range(i):
            seen = vis(i, j)
            acc = acc + (g[j] if seen is None else seen * g[j])
        gam.append(acc)
    eg = [jnp.exp(x) for x in gam]

    def decay(i, j):
        value = jnp.exp(jnp.minimum(gam[i] - gam[j], 0.0))
        seen = vis(i, j)
        return value if seen is None else value * seen

    def gram(i, j):
        return jnp.sum(kt_ref[i] * kt_ref[j], axis=0, keepdims=True) * (inv[i] * inv[j])

    dec = {(i, j): decay(i, j) for i in range(positions) for j in range(i)}
    coupling = {(i, j): beta[i] * gram(i, j) * dec[i, j] for (i, j) in dec}
    reach = {}
    for p in range(prop):
        i = prop + p
        for j in range(i + 1):
            value = gram(positions + p, j)
            reach[p, j] = value if j == i else value * dec[i, j]

    last = eg[prop - 1]
    eg_ref[...] = jnp.broadcast_to(last, (lanes, lanes)).T

    lane = lax.broadcasted_iota(jnp.int32, (vdim, lanes), 1)
    inner, outer = lane % GROUP, lane // GROUP
    products = []
    for c in range(groups):
        rows = s_ref[c * GROUP : (c + 1) * GROUP, 0].reshape(GROUP * vdim, hd).astype(bf16)
        tiles = []
        for ref in (ok_ref, k_ref, q_ref):
            for p in range(prop):
                start = p * lanes + c * GROUP
                tiles.append(ref[start : start + GROUP, :])
        keys = jnp.concatenate(tiles, axis=0)
        product = lax.dot_general(
            rows, keys, (((1,), (1,)), ((), ())), preferred_element_type=f32
        )
        wide = []
        for first in range(0, 3 * prop * GROUP, lanes):
            width = min(lanes, 3 * prop * GROUP - first)
            part = product[:, first : first + width]
            chosen = part[:vdim]
            for s in range(1, GROUP):
                mask = (inner if width == lanes else inner[:, :width]) == s
                chosen = jnp.where(mask, part[s * vdim : (s + 1) * vdim], chosen)
            if width < lanes:
                chosen = jnp.concatenate(
                    [chosen, jnp.zeros((vdim, lanes - width), f32)], axis=1
                )
            wide.append(chosen)
        products.append(wide)

    per_tile = lanes // GROUP

    def swap(source, sources, targets):
        shifted = []
        for d in range(groups):
            acc = None
            for a in range(sources):
                t = (a - d) % groups
                if t >= targets:
                    continue
                acc = source[a] if acc is None else jnp.where(outer == t, source[a], acc)
            shifted.append(acc if acc is None or d == 0 else pltpu.roll(acc, d * GROUP, 1))
        results = []
        for t in range(targets):
            acc = None
            for a in range(sources):
                piece = shifted[(a - t) % groups]
                acc = piece if acc is None else jnp.where(outer == a, piece, acc)
            results.append(acc)
        return results

    raw = []
    for tile in range(len(products[0])):
        count = min(per_tile, 3 * prop - tile * per_tile)
        raw += swap([products[c][tile] for c in range(groups)], groups, count)

    update = []
    for i in range(positions):
        source = ov_ref if i < prop else v_ref
        p = i % prop
        value = source[:, p * lanes : (p + 1) * lanes].astype(f32)
        acc = beta[i] * value - (beta[i] * eg[i] * inv[i]) * raw[i]
        for j in range(i):
            acc = acc - coupling[i, j] * update[j]
        update.append(acc)

    for p in range(prop):
        i = prop + p
        acc = (eg[i] * inv[positions + p]) * raw[positions + p]
        for j in range(i + 1):
            acc = acc + reach[p, j] * update[j]
        o_ref[0, :, p * lanes : (p + 1) * lanes] = acc
        sq_ref[0, :, p * lanes : (p + 1) * lanes] = jnp.sum(acc * acc, axis=0, keepdims=True)

    weighted = [
        update[j] * (jnp.exp(gam[prop - 1] - gam[j]) * inv[j]) for j in range(prop)
    ]
    compact = swap(weighted, prop, groups)
    width = prop * GROUP
    narrow = inner[:, :width]
    for c in range(groups):
        tiles = [
            ok_ref[p * lanes + c * GROUP : p * lanes + (c + 1) * GROUP, :] for p in range(prop)
        ]
        keys = jnp.concatenate(tiles, axis=0)
        piece = compact[c][:, :width]
        left = jnp.concatenate(
            [jnp.where(narrow == s, piece, 0.0) for s in range(GROUP)], axis=0
        ).astype(bf16)
        delta = jnp.dot(left, keys, preferred_element_type=f32)
        for s in range(GROUP):
            seq = c * GROUP + s
            out_ref[seq, 0] = (
                s_ref[seq, 0] * eg_ref[seq : seq + 1, :hd] + delta[s * vdim : (s + 1) * vdim]
            )


def delta_call(prop, lanes, q, k, ok, v, ov, scal, state):
    seqs, heads, vdim, hd = state.shape
    tiles = seqs // lanes
    block = prop * lanes
    natural = pl.BlockSpec((block, hd), lambda t, h: (t, h))
    turned = pl.BlockSpec((vdim, block), lambda t, h: (h, t))
    state_spec = pl.BlockSpec((lanes, 1, vdim, hd), lambda t, h: (t, h, 0, 0))
    return pl.pallas_call(
        functools.partial(delta_kernel, prop),
        grid=(tiles, heads),
        in_specs=[
            natural,
            natural,
            natural,
            turned,
            turned,
            pl.BlockSpec((1, 8, block), lambda t, h: (h, 0, t)),
            state_spec,
        ],
        out_specs=[
            pl.BlockSpec((1, vdim, block), lambda t, h: (h, 0, t)),
            pl.BlockSpec((1, 1, block), lambda t, h: (h, 0, t)),
            state_spec,
        ],
        out_shape=[
            jax.ShapeDtypeStruct((heads, vdim, seqs * prop), jnp.float32),
            jax.ShapeDtypeStruct((heads, 1, seqs * prop), jnp.float32),
            jax.ShapeDtypeStruct(state.shape, jnp.float32),
        ],
        scratch_shapes=[
            pltpu.VMEM((3 * prop, hd, lanes), jnp.float32),
            pltpu.VMEM((lanes, lanes), jnp.float32),
        ],
        compiler_params=pltpu.CompilerParams(vmem_limit_bytes=40 * 1024 * 1024),
        cost_estimate=pl.CostEstimate(
            flops=2 * seqs * heads * vdim * hd * 256,
            bytes_accessed=8 * seqs * heads * vdim * hd,
            transcendentals=0,
        ),
    )(q, k, ok, v, ov, scal, state)


def scattered_sum(blended, weight, own):
    f32, bf16 = jnp.float32, jnp.bfloat16
    channels, rows = blended.shape
    kv, tp = lax.axis_size("kv"), lax.axis_size("tp")
    chips = tp // 2
    core = lax.axis_index("tp") % 2
    halves = weight.reshape(channels, kv * chips, 2, own)

    def half(which):
        part = lax.dynamic_index_in_dim(halves, which, 2, keepdims=False)
        return lax.dot_general(
            part.reshape(channels, kv * chips * own),
            blended,
            (((0,), (0,)), ((), ())),
            preferred_element_type=f32,
        )

    pairs = [(i, i ^ 1) for i in range(tp)]
    received = lax.ppermute(half(1 - core).astype(bf16), "tp", pairs)
    summed = (half(core) + received.astype(f32)).astype(bf16).reshape(kv, chips, own, rows)
    if chips == 2:
        x = lax.axis_index("tp") // 2
        across = [(i, i ^ 2) for i in range(tp)]
        other = lax.dynamic_index_in_dim(summed, 1 - x, 1, keepdims=False)
        mine = lax.dynamic_index_in_dim(summed, x, 1, keepdims=False)
        other = lax.ppermute(other, "tp", across)
        summed = (mine.astype(f32) + other.astype(f32)).astype(bf16)
    else:
        groups = [[2 * x + c for x in range(chips)] for c in range(2)]
        parts = lax.all_to_all(summed, "tp", 1, 1, axis_index_groups=groups, tiled=True)
        summed = jnp.sum(parts.astype(f32), axis=1).astype(bf16)
    parts = lax.all_to_all(summed, "kv", 0, 0, tiled=True)
    return jnp.sum(parts.astype(f32), axis=0)


def on_device(
    tokens,
    input_norm_gain,
    query_weight,
    key_weight,
    value_weight,
    output_gate_weight,
    strength_weight,
    decay_weight,
    head_decay_rate,
    proposal_log_decay,
    head_norm_gain,
    output_weight,
    output_norm_gain,
    state,
    previous_keys,
    previous_values,
    previous_log_decay,
    previous_strengths,
    accepted,
    parent,
):
    f32, bf16 = jnp.float32, jnp.bfloat16
    seqs, heads, vdim, hd = state.shape
    prop = parent.shape[1]
    rows = seqs * prop
    width = input_norm_gain.shape[0]
    lanes = min(128, seqs)
    tiles = seqs // lanes

    def order(x):
        tail = x.shape[2:]
        x = x.reshape((tiles, lanes, prop) + tail)
        return x.swapaxes(1, 2).reshape((rows,) + tail)

    own = tokens.shape[2]
    gathered = lax.all_gather(order(tokens), AXES, axis=1, tiled=True)
    features = gathered.astype(f32)
    normed = features * lax.rsqrt(jnp.mean(features * features, axis=-1, keepdims=True) + epsilon)
    normed = (normed * input_norm_gain.astype(f32)).astype(bf16)

    queries = jnp.dot(normed, query_weight, preferred_element_type=f32).astype(bf16)
    keys = jnp.dot(normed, key_weight, preferred_element_type=f32).astype(bf16)
    small = jnp.concatenate(
        [
            value_weight.reshape(width, -1),
            output_gate_weight.reshape(width, -1),
            strength_weight,
            decay_weight,
        ],
        axis=1,
    )
    side = lax.dot_general(
        small, normed, (((0,), (1,)), ((), ())), preferred_element_type=f32
    )
    channels = heads * vdim
    values = side[:channels].astype(bf16)
    zgate = side[channels : 2 * channels].astype(bf16).astype(f32)
    strength = side[2 * channels : 2 * channels + heads]
    decay_pre = side[2 * channels + heads :]

    beta_new = jax.nn.sigmoid(strength)
    g_new = -head_decay_rate[:, None] * jax.nn.softplus(decay_pre) + order(proposal_log_decay).T
    position = jnp.arange(prop, dtype=jnp.int32)
    live = (position[None, :] < accepted[:, None]).astype(f32)[:, :, None]
    beta_old = order(previous_strengths * live).T
    g_old = order(previous_log_decay * live).T
    parents = jnp.broadcast_to(order(parent).astype(f32)[None], (heads, rows))
    zero = jnp.zeros((heads, rows), f32)
    scal = jnp.stack([beta_old, g_old, beta_new, g_new, parents, zero, zero, zero], axis=1)
    old_keys = order(previous_keys)
    old_values = order(previous_values).reshape(rows, channels).T

    readout, squares, accepted_state = delta_call(
        prop, lanes, queries, keys, old_keys, values, old_values, scal, state
    )
    squares = lax.psum(squares.reshape(heads, rows), "tp")
    scale = lax.rsqrt(squares / hd + epsilon)[:, None, :]
    blended = readout * scale * head_norm_gain.astype(f32)[None, :, None]
    blended = blended * jax.nn.silu(zgate).reshape(heads, vdim, rows)
    blended = blended.reshape(channels, rows).astype(bf16)
    share = scattered_sum(blended, output_weight.reshape(channels, width), own)
    sumsq = lax.psum(jnp.sum(share * share, axis=0), AXES)
    scaling = lax.rsqrt(sumsq / width + epsilon)[None, :]
    layer_out = (share * scaling * output_norm_gain.astype(f32)[:, None]).astype(bf16).T
    layer_out = layer_out.reshape(tiles, prop, lanes, own).swapaxes(1, 2)
    return (layer_out.reshape(seqs, prop, own), accepted_state)


def solution(mesh):
    placed = (
        P(None, None, AXES),
        P(),
        P(None, "kv"),
        P(None, "kv"),
        P(None, "kv", "tp"),
        P(None, "kv", "tp"),
        P(None, "kv"),
        P(None, "kv"),
        P("kv"),
        P(None, None, "kv"),
        P("tp"),
        P("kv", "tp", None),
        P(AXES),
        P(None, "kv", "tp", None),
        P(None, None, "kv"),
        P(None, None, "kv", "tp"),
        P(None, None, "kv"),
        P(None, None, "kv"),
        P(),
        P(),
    )
    return jax.shard_map(
        on_device,
        mesh=mesh,
        in_specs=placed,
        out_specs=(P(None, None, AXES), P(None, "kv", "tp", None)),
        check_vma=False,
    )
```
